32 devices in a mesh: sp: 8 (over z, x), tp: 4 (over y, core).
Axes of the slice: x: 2, y: 2, z: 4, core: 2. Of those that a mesh axis runs over, the one named last changes fastest.
Arguments:
- resid: bfloat16 [2048, 4096], P(('sp', 'tp')), may hold values from -6 to 6
- queries: bfloat16 [2048, 2048], P('sp', 'tp'), may hold values from -6 to 6
- keys: bfloat16 [2048, 512], P('sp', 'tp'), may hold values from -6 to 6
- values: bfloat16 [2048, 512], P('sp', 'tp'), may hold values from -6 to 6
- q_gain: float32 [128], replicated, may hold values from 0.5 to 6
- key_norm_gain: float32 [128], replicated, may hold values from 0.5 to 6
- out_weight: bfloat16 [2048, 4096], P('tp'), may hold values from -0.125 to 0.125
- norm1_gain: float32 [4096], replicated, may hold values from 0.1 to 1.9
- norm2_gain: float32 [4096], replicated, may hold values from 0.1 to 1.9
- expert_ids: int32 [2048, 2], P(('sp', 'tp')), may hold values from 0 to 7, all different within a row; in each aligned block of 64 rows (0 to 63, 64 to 127, ...) at most 24 rows name the same one
- group_weight: float32 [2048], P(('sp', 'tp')), may hold values from 0.3 to 1
- expert_weight: float32 [2048, 2], P(('sp', 'tp')), may hold values from 0.1 to 1
- gate_proj: bfloat16 [8, 4096, 1024], P('sp', None, 'tp'), may hold values from -0.09375 to 0.09375
- up_proj: bfloat16 [8, 4096, 1024], P('sp', None, 'tp'), may hold values from -0.09375 to 0.09375
- down_proj: bfloat16 [8, 1024, 4096], P('sp', 'tp'), may hold values from -0.1875 to 0.1875
Outputs:
- mixed_out: bfloat16 [2048, 4096], P(('sp', 'tp'))
The draws below stay inside these ranges and needn't reach their ends.
Inputs may be any that keep to these rules, and one draw needn't show every extreme that they name: `expert_ids`: each row names 2 different experts. Among the rows of one device (aligned blocks of 64 rows) no expert is named by more than 24 rows, a bound that some block reaches.
All inputs are finite; a program needn't handle non-finite values.
Results may differ from the reference program's by a relative error of at most 0.012.
The reference program's roundings to bfloat16 on the way count: a program that leaves them out, or rounds other values in their place, can miss the bound.
Values may be sent and summed in bfloat16 or wider, within the bound.
No kernel may reach another device: no remote copies, remote signals or barrier semaphores. Data moves between devices by JAX's collectives and lax.ppermute only.
A program may use at most 192 MiB of HBM per device.

```python
import math
import jax
import jax.numpy as jnp
import numpy as np
from jax import lax

D = 4096
HEAD_WIDTH = 128
QUERY_HEADS = 16
KEY_VALUE_HEADS = 4
GRID_W = 64
FF = 1024
TOP = 2
SEQUENCE_TOKENS = 2048
ROWS_DEV = 64
EXPERTS = 8
CAP = 24
N_SP = 8
N_TP = 4


def gain_law(key):
    return jax.random.uniform(key, (HEAD_WIDTH,), jnp.float32, 0.5, 2.0)


def draw_q_gain(key, part):
    return gain_law(jax.random.fold_in(key, 31))


def draw_key_norm_gain(key, part):
    return gain_law(jax.random.fold_in(key, 37))


def key_table(key):
    sampled_values = jax.random.normal(jax.random.fold_in(key, 41), (SEQUENCE_TOKENS, KEY_VALUE_HEADS * HEAD_WIDTH), jnp.float32)
    return jnp.clip(sampled_values, -6.0, 6.0)


def draw_keys(key, part):
    return key_table(key).astype(jnp.bfloat16)


def draw_queries(key, part):
    sampled_values = jax.random.normal(jax.random.fold_in(key, 43), (SEQUENCE_TOKENS, QUERY_HEADS * HEAD_WIDTH), jnp.float32)
    sampled_values = jnp.clip(sampled_values, -6.0, 6.0)
    return sampled_values.astype(jnp.bfloat16)


def block_scale(stream_key, shape, split, low, high):
    def one(dim, parts):
        draws = jax.random.uniform(jax.random.fold_in(jax.random.fold_in(stream_key, 6), dim), (parts,), jnp.float32, low / len(split), high / len(split))
        return jnp.repeat(jnp.exp(draws), shape[dim] // parts).reshape((-1,) + (1,) * (len(shape) - dim - 1))

    loudness = one(*split[0])
    for cut in split[1:]:
        loudness = loudness * one(*cut)
    return loudness


def routed_block(own_key, own, number, rows, amount, top, reach, lean):
    ranking = jax.random.permutation(own_key, amount)
    heavy_load, common = load_shares(amount, rows * top, reach, lean, True), load_shares(amount, rows * top, reach, lean, False)
    places = jnp.arange(amount)

    def named(tallies, turn):
        used = int((tallies > 0).sum())
        fixed = max(1, used // 4)
        shifted = fixed + (places - fixed + turn * (used - fixed)) % max(1, amount - fixed)
        return jnp.zeros((amount,), jnp.int32).at[ranking[jnp.where(places < fixed, places, shifted)]].set(jnp.asarray(tallies, jnp.int32))

    tallies = jnp.where(number % 4 == 0, named(heavy_load, number // 4), named(common, number - number // 4 - 1))
    mixed = jax.random.permutation(jax.random.fold_in(own, 3), amount)
    donor, sink = mixed[0:amount // 2 * 2:2], mixed[1:amount // 2 * 2:2]
    slack = jnp.minimum(tallies[donor] - 1, reach - tallies[sink]) // 2
    slack = jnp.where((donor == ranking[0]) | (sink == ranking[0]) | (tallies[sink] == 0), 0, jnp.maximum(slack, 0))
    shifted = jax.random.randint(jax.random.fold_in(own, 4), (amount // 2,), 0, 1 << 20) % (slack + 1)
    tallies = tallies.at[donor].add(-shifted).at[sink].add(shifted)
    items = jnp.searchsorted(jnp.cumsum(tallies), jnp.arange(rows * top), side="right").astype(jnp.int32)
    table = items.reshape(top, rows).T
    table = table[jax.random.permutation(jax.random.fold_in(own, 1), rows)]
    turn = jax.random.randint(jax.random.fold_in(own, 2), (rows, 1), 0, top)
    return jnp.take_along_axis(table, (jnp.arange(top)[None, :] + turn) % top, axis=1)


def load_shares(count, total, bound, skew, full):
    weights = [(1 << 20) // math.isqrt(grade ** skew) + 1 for grade in range(1, count + 1)]
    largest = bound if full else min(bound, max(-(-total // count), total * weights[0] // sum(weights)))
    least = 1 if total - largest >= count - 1 else 0
    holding, surplus = [largest] + [least] * (count - 1), total - largest - least * (count - 1)
    while surplus > 0:
        free = [i for i in range(1, count) if holding[i] < largest] or [i for i in range(1, count) if holding[i] < bound]
        whole, left = sum([weights[i] for i in free]), surplus
        for i in free:
            more = min(bound - holding[i], max(1, left * weights[i] // whole), surplus)
            holding[i] = holding[i] + more
            surplus = surplus - more
    return np.array(holding)


def normal_values(rng, dims, deviation, bound, split=(), kind=jnp.bfloat16):
    values = deviation * jax.random.normal(rng, dims, jnp.float32)
    if split:
        values = values * block_scale(rng, dims, split, -0.22, 0.18)
    return jnp.clip(values, -bound, bound).astype(kind)


def setup_inputs(seed: int = 0) -> dict:
    streams_of = jax.random.split(jax.random.key(seed), 16)
    resid = normal_values(streams_of[0], (SEQUENCE_TOKENS, D), 1.0, 6.0, ((0, 32),))
    queries = draw_queries(jax.random.fold_in(streams_of[15], 71), 0)
    keys = draw_keys(jax.random.fold_in(streams_of[15], 71), 0)
    values = normal_values(streams_of[3], (SEQUENCE_TOKENS, KEY_VALUE_HEADS * HEAD_WIDTH), 1.0, 6.0, ((0, 8), (1, 4)))
    q_gain = draw_q_gain(jax.random.fold_in(streams_of[15], 71), 0)
    key_norm_gain = draw_key_norm_gain(jax.random.fold_in(streams_of[15], 71), 0)
    out_weight = normal_values(streams_of[6], (QUERY_HEADS * HEAD_WIDTH, D), (QUERY_HEADS * HEAD_WIDTH) ** -0.5, 0.125, ((0, 4),))
    norm1_gain = jnp.clip(1.0 + 0.18 * jax.random.normal(streams_of[7], (D,), jnp.float32), 0.1, 1.9)
    norm2_gain = jnp.clip(1.0 + 0.18 * jax.random.normal(streams_of[8], (D,), jnp.float32), 0.1, 1.9)
    expert_ids_keys = jax.random.split(jax.random.fold_in(streams_of[9], 1), SEQUENCE_TOKENS // ROWS_DEV)
    expert_ids_turns = jax.random.permutation(jax.random.fold_in(streams_of[9], 3), SEQUENCE_TOKENS // ROWS_DEV)
    expert_ids = jax.vmap(lambda own, number: routed_block(jax.random.fold_in(streams_of[9], 2), own, number, ROWS_DEV, EXPERTS, TOP, CAP, 1))(expert_ids_keys, expert_ids_turns).reshape((SEQUENCE_TOKENS, TOP))
    group_weight = jnp.clip(0.3 + 0.7 * jax.random.uniform(streams_of[10], (SEQUENCE_TOKENS,), jnp.float32) ** block_scale(streams_of[10], (SEQUENCE_TOKENS,), ((0, 32),), -0.2, 0.2), 0.3, 1.0)
    expert_weight = jnp.clip(0.1 + 0.9 * jax.random.uniform(streams_of[11], (SEQUENCE_TOKENS, TOP), jnp.float32) ** block_scale(streams_of[11], (SEQUENCE_TOKENS, TOP), ((0, 32),), -0.2, 0.2), 0.1, 1.0)
    gate_proj = normal_values(streams_of[12], (EXPERTS, D, FF), D ** -0.5, 0.09375, ((0, 8), (2, 4)))
    up_proj = normal_values(streams_of[13], (EXPERTS, D, FF), D ** -0.5, 0.09375, ((0, 8), (2, 4)))
    down_proj = normal_values(streams_of[14], (EXPERTS, FF, D), FF ** -0.5, 0.1875, ((0, 8), (1, 4)))
    return dict(resid=resid, queries=queries, keys=keys, values=values, q_gain=q_gain, key_norm_gain=key_norm_gain, out_weight=out_weight, norm1_gain=norm1_gain, norm2_gain=norm2_gain, expert_ids=expert_ids, group_weight=group_weight, expert_weight=expert_weight, gate_proj=gate_proj, up_proj=up_proj, down_proj=down_proj)


deep_alpha = 2.0 ** 0.5
rope_theta = 10000.0

def apply_rotary_heads(block, gain, grid_positions):
    values32 = block.astype(jnp.float32)
    normed = values32 * lax.rsqrt(lax.optimization_barrier(jnp.mean(values32 * values32, -1, keepdims=True)) + 1e-06) * gain
    half = normed.shape[-1] // 2
    inv_freq = rope_theta ** (-jnp.arange(0, half, 2, dtype=jnp.float32) / half)
    grid_row = (grid_positions // GRID_W).astype(jnp.float32)
    grid_col = (grid_positions % GRID_W).astype(jnp.float32)
    angle = jnp.concatenate([grid_row[:, None] * inv_freq, grid_col[:, None] * inv_freq], -1)[:, None, :]
    cosine = jnp.cos(angle)
    sine = jnp.sin(angle)
    first = normed[..., :half]
    second = normed[..., half:]
    turned = jnp.concatenate([first * cosine - second * sine, first * sine + second * cosine], -1)
    return turned.astype(jnp.bfloat16)

def layer_norm_gain(summed, gain):
    centre = summed - lax.optimization_barrier(jnp.mean(summed, -1, keepdims=True))
    spread = lax.optimization_barrier(jnp.mean(centre * centre, -1, keepdims=True))
    return centre * lax.rsqrt(spread + 1e-06) * gain

def reference(resid, queries, keys, values, q_gain, key_norm_gain, out_weight, norm1_gain, norm2_gain, expert_ids, group_weight, expert_weight, gate_proj, up_proj, down_proj):
    grid_positions = jnp.arange(SEQUENCE_TOKENS, dtype=jnp.int32)
    query_group = QUERY_HEADS // KEY_VALUE_HEADS
    q_rot = apply_rotary_heads(queries.reshape(SEQUENCE_TOKENS, QUERY_HEADS, HEAD_WIDTH), q_gain, grid_positions)
    rotated_keys = apply_rotary_heads(keys.reshape(SEQUENCE_TOKENS, KEY_VALUE_HEADS, HEAD_WIDTH), key_norm_gain, grid_positions).astype(jnp.float32)
    value_rows_full = values.reshape(SEQUENCE_TOKENS, KEY_VALUE_HEADS, HEAD_WIDTH).astype(jnp.float32)
    query_extent = math.gcd(SEQUENCE_TOKENS, 128)

    def attend(query_tile):
        query_widened = query_tile.reshape(query_extent, KEY_VALUE_HEADS, query_group, HEAD_WIDTH).astype(jnp.float32)
        scores = jnp.einsum('qkgd,lkd->kgql', query_widened, rotated_keys) * HEAD_WIDTH ** (-0.5)
        row_max = lax.optimization_barrier(jnp.max(scores, -1, keepdims=True))
        weights = jnp.exp(scores - row_max)
        row_sum = lax.optimization_barrier(jnp.sum(weights, -1))
        rounded = lax.optimization_barrier(weights.astype(jnp.bfloat16)).astype(jnp.float32)
        mixed = jnp.einsum('kgql,lkd->qkgd', rounded, value_rows_full)
        mixed = mixed / jnp.transpose(row_sum, (2, 0, 1))[..., None]
        return mixed.reshape(query_extent, QUERY_HEADS * HEAD_WIDTH).astype(jnp.bfloat16)
    attn = lax.map(attend, q_rot.reshape(SEQUENCE_TOKENS // query_extent, query_extent, QUERY_HEADS, HEAD_WIDTH)).reshape(SEQUENCE_TOKENS, QUERY_HEADS * HEAD_WIDTH)
    proj = jnp.dot(attn, out_weight, preferred_element_type=jnp.float32).astype(jnp.bfloat16)
    summed = deep_alpha * resid.astype(jnp.float32) + proj.astype(jnp.float32)
    x_one = layer_norm_gain(summed, norm1_gain).astype(jnp.bfloat16)
    gates = group_weight[:, None] * expert_weight / lax.optimization_barrier(jnp.sum(expert_weight, -1, keepdims=True))
    copies = SEQUENCE_TOKENS * TOP
    most_rows = CAP * N_SP * N_TP
    ff_dev = FF // N_TP
    flat_ids = expert_ids.reshape(-1)
    gate_flat = jnp.concatenate([gates.reshape(-1), jnp.zeros((1,), jnp.float32)])
    x_padded = jnp.concatenate([x_one, jnp.zeros((1, D), jnp.bfloat16)], 0)

    def per_expert(total, expert):
        index = jnp.nonzero(flat_ids == expert, size=most_rows, fill_value=copies)[0].astype(jnp.int32)
        token_index = jnp.where(index < copies, index // TOP, SEQUENCE_TOKENS).astype(jnp.int32)
        chosen = x_padded[token_index]
        w_gate = lax.dynamic_index_in_dim(gate_proj, expert, 0, keepdims=False)
        w_up = lax.dynamic_index_in_dim(up_proj, expert, 0, keepdims=False)
        w_down = lax.dynamic_index_in_dim(down_proj, expert, 0, keepdims=False)
        gate_part = jnp.dot(chosen, w_gate, preferred_element_type=jnp.float32)
        up_part = jnp.dot(chosen, w_up, preferred_element_type=jnp.float32)
        hidden = (jax.nn.silu(gate_part) * up_part).astype(jnp.bfloat16)
        expert_sum = jnp.zeros((most_rows, D), jnp.float32)
        for lane in range(N_TP):
            partial_sum = jnp.dot(hidden[:, lane * ff_dev:(lane + 1) * ff_dev], w_down[lane * ff_dev:(lane + 1) * ff_dev], preferred_element_type=jnp.float32)
            rounded = lax.optimization_barrier(partial_sum.astype(jnp.bfloat16))
            expert_sum = expert_sum + rounded.astype(jnp.float32)
        expert_out = expert_sum.astype(jnp.bfloat16).astype(jnp.float32)
        weighted = gate_flat[index][:, None] * expert_out
        return (total.at[token_index].add(weighted), None)
    start_total = jnp.zeros((SEQUENCE_TOKENS + 1, D), jnp.float32)
    moe_total, _ = lax.scan(per_expert, start_total, jnp.arange(EXPERTS, dtype=jnp.int32))
    moe = moe_total[:SEQUENCE_TOKENS]
    final = deep_alpha * x_one.astype(jnp.float32) + moe
    return layer_norm_gain(final, norm2_gain).astype(jnp.bfloat16)
```

```python
import functools
import math

import jax
import jax.numpy as jnp
from jax import lax
from jax.experimental import pallas as pl
from jax.experimental.pallas import tpu as pltpu
from jax.sharding import PartitionSpec as P

GRID_W = 64


deep_alpha = 2.0**0.5
rope_theta = 10000.0


def swap(block, axis, bits):
    if bits == 0:
        return block
    count = lax.axis_size(axis)
    return lax.ppermute(block, axis, [(i, i ^ bits) for i in range(count)])


def rotary_angles(head_size, grid_positions):
    half = head_size // 2
    inv_freq = rope_theta ** (-jnp.arange(0, half, 2, dtype=jnp.float32) / half)
    grid_row = (grid_positions // GRID_W).astype(jnp.float32)
    grid_col = (grid_positions % GRID_W).astype(jnp.float32)
    angle = jnp.concatenate([grid_row[:, None] * inv_freq, grid_col[:, None] * inv_freq], -1)
    return jnp.cos(angle), jnp.sin(angle)


def apply_rotary_heads(block, gain, cosine, sine):
    values32 = block.astype(jnp.float32)
    normed = values32 * lax.rsqrt(jnp.mean(values32 * values32, -1, keepdims=True) + 1e-06) * gain
    half = normed.shape[-1] // 2
    cosine = cosine[..., None, :]
    sine = sine[..., None, :]
    first = normed[..., :half]
    second = normed[..., half:]
    turned = jnp.concatenate([first * cosine - second * sine, first * sine + second * cosine], -1)
    return turned.astype(jnp.bfloat16)


def layer_norm_gain(summed, gain):
    centre = summed - jnp.mean(summed, -1, keepdims=True)
    spread = jnp.mean(centre * centre, -1, keepdims=True)
    return centre * lax.rsqrt(spread + 1e-06) * gain


def attention_kernel(scale, chunks, *refs):
    query_ref = refs[0]
    key_refs = refs[1 : 1 + chunks]
    value_refs = refs[1 + chunks : 1 + 2 * chunks]
    out_ref = refs[1 + 2 * chunks]
    query = query_ref[...]
    scores = [
        lax.dot_general(
            query, key[...], (((1,), (1,)), ((), ())), preferred_element_type=jnp.float32
        )
        * scale
        for key in key_refs
    ]
    row_max = functools.reduce(jnp.maximum, [jnp.max(s, -1, keepdims=True) for s in scores])
    row_sum = jnp.zeros_like(row_max)
    weighted = jnp.zeros(out_ref.shape, jnp.float32)
    for block, value in zip(scores, value_refs):
        probs = jnp.exp(block - row_max)
        row_sum = row_sum + jnp.sum(probs, -1, keepdims=True)
        weighted = weighted + jnp.dot(
            probs.astype(jnp.bfloat16), value[...], preferred_element_type=jnp.float32
        )
    out_ref[...] = (weighted / row_sum).astype(out_ref.dtype)


def attention(query, pieces, kv_local, head_size):
    rows, width = query.shape
    heads = width // head_size
    group = heads // kv_local
    scale = head_size ** (-0.5)
    count = len(pieces)
    tokens = pieces[0].shape[0]
    block_rows = math.gcd(rows, 256)
    query_spec = pl.BlockSpec((block_rows, head_size), lambda h, r: (r, h))
    key_spec = pl.BlockSpec((tokens, head_size), lambda h, r: (0, h // group))
    value_spec = pl.BlockSpec((tokens, head_size), lambda h, r: (0, kv_local + h // group))
    return pl.pallas_call(
        functools.partial(attention_kernel, scale, count),
        grid=(heads, rows // block_rows),
        in_specs=[query_spec] + [key_spec] * count + [value_spec] * count,
        out_specs=query_spec,
        out_shape=jax.ShapeDtypeStruct((rows, width), jnp.bfloat16),
        compiler_params=pltpu.CompilerParams(
            dimension_semantics=("arbitrary", "arbitrary"), vmem_limit_bytes=48 * 1024 * 1024
        ),
        name="attention",
    )(query, *pieces, *pieces)


def gather_swapped(block, axis):
    count = lax.axis_size(axis)
    got = {0: block}
    for bits in range(0, count, 2):
        got[bits] = swap(block, axis, bits)
        got[bits ^ 1] = swap(got[bits], axis, 1)
    return [got[i] for i in range(count)]


def gather_tp(block):
    have = [block]
    step = lax.axis_size("tp") // 2
    found = {0: block}
    while step:
        for key in list(found):
            found[key ^ step] = swap(found[key], "tp", step)
        step //= 2
    return [found[i] for i in range(lax.axis_size("tp"))]


def scatter_sum_tp(parts):
    step = 1
    parts = dict(enumerate(parts))
    while len(parts) > 1:
        sent = {k: swap(v.astype(jnp.bfloat16), "tp", step) for k, v in parts.items() if k & step}
        parts = {
            k: v.astype(jnp.bfloat16).astype(jnp.float32) + sent[k | step].astype(jnp.float32)
            for k, v in parts.items()
            if not k & step
        }
        step *= 2
    return parts[0]


def per_device(
    resid,
    queries,
    keys,
    values,
    q_gain,
    key_norm_gain,
    out_weight,
    norm1_gain,
    norm2_gain,
    expert_ids,
    group_weight,
    expert_weight,
    gate_proj,
    up_proj,
    down_proj,
):
    local_tokens = queries.shape[0]
    head_size = q_gain.shape[0]
    kv_local = keys.shape[1] // head_size
    heads = queries.shape[1] // head_size
    model_width = resid.shape[1]
    sp_count = lax.axis_size("sp")
    lanes = lax.axis_size("tp")
    own_rows = local_tokens // lanes
    own_sp = lax.axis_index("sp")
    own_tp = lax.axis_index("tp")

    positions = own_sp * local_tokens + jnp.arange(local_tokens, dtype=jnp.int32)
    cosine, sine = rotary_angles(head_size, positions)
    rotated_keys = apply_rotary_heads(
        keys.reshape(local_tokens, kv_local, head_size), key_norm_gain, cosine, sine
    ).reshape(local_tokens, kv_local * head_size)
    pieces = gather_swapped(jnp.concatenate([rotated_keys, values], -1), "sp")
    per = max(1, sp_count // 8)
    pieces = [jnp.concatenate(pieces[i : i + per]) if per > 1 else pieces[i] for i in range(0, sp_count, per)]

    order = own_tp ^ jnp.arange(lanes, dtype=jnp.int32)

    def reorder(array):
        return array.reshape((lanes, own_rows) + array.shape[1:])[order].reshape(array.shape)

    q_rot = apply_rotary_heads(
        reorder(queries).reshape(local_tokens, heads, head_size),
        q_gain,
        reorder(cosine),
        reorder(sine),
    ).reshape(local_tokens, heads * head_size)

    top_count = expert_ids.shape[1]
    expert_local = gate_proj.shape[0]
    expert_total = expert_local * sp_count
    capacity = (3 * top_count * own_rows + 2 * expert_total - 1) // (2 * expert_total)
    flat_ids = expert_ids.reshape(-1)
    one_hot = (flat_ids[:, None] == jnp.arange(expert_total, dtype=jnp.int32)[None, :]).astype(
        jnp.float32
    )
    places = jnp.arange(flat_ids.shape[0], dtype=jnp.int32)
    before = (places[None, :] < places[:, None]).astype(jnp.float32)
    rank = jnp.sum(jnp.dot(before, one_hot) * one_hot, 1).astype(jnp.int32)
    swapped_ids = (flat_ids // expert_local ^ own_sp) * expert_local + flat_ids % expert_local
    slot = (swapped_ids * capacity + rank).reshape(own_rows, top_count)
    slots = expert_total * capacity
    hit = slot[..., None] == jnp.arange(slots, dtype=jnp.int32)
    placing = jnp.sum(hit.astype(jnp.float32), 1).astype(jnp.bfloat16)
    gates = group_weight[:, None] * expert_weight / jnp.sum(expert_weight, -1, keepdims=True)
    mixing = jnp.sum(jnp.where(hit, gates[..., None], 0.0), 1)
    mixing_high = mixing.astype(jnp.bfloat16)
    mixing_low = (mixing - mixing_high.astype(jnp.float32)).astype(jnp.bfloat16)
    mixing = jnp.concatenate([mixing_high, mixing_low])

    attn = attention(q_rot, pieces, kv_local, head_size)
    partial = [
        jnp.dot(
            attn[i * own_rows : (i + 1) * own_rows], out_weight, preferred_element_type=jnp.float32
        )
        for i in range(lanes)
    ]
    proj = scatter_sum_tp(partial).astype(jnp.bfloat16)
    summed = deep_alpha * resid.astype(jnp.float32) + proj.astype(jnp.float32)
    x_one = layer_norm_gain(summed, norm1_gain).astype(jnp.bfloat16)

    outgoing = lax.dot_general(
        placing, x_one, (((0,), (0,)), ((), ())), preferred_element_type=jnp.float32
    ).astype(jnp.bfloat16)
    slab = expert_local * capacity
    groups = min(4, sp_count)
    per_group = sp_count // groups
    arrived = [swap(outgoing[d * slab : (d + 1) * slab], "sp", d) for d in range(sp_count)]
    returned = [None] * sp_count
    for g in range(groups):
        members = range(g * per_group, (g + 1) * per_group)
        block = jnp.concatenate([arrived[d] for d in members])
        rows = block.shape[0]
        piece = jnp.concatenate(gather_tp(block))
        total = piece.shape[0]
        by_expert = piece.reshape(total // slab, expert_local, capacity, model_width)
        outs = []
        for e in range(expert_local):
            tokens = by_expert[:, e].reshape(total // expert_local, model_width)
            gate_part = jnp.dot(tokens, gate_proj[e], preferred_element_type=jnp.float32)
            up_part = jnp.dot(tokens, up_proj[e], preferred_element_type=jnp.float32)
            hidden = (jax.nn.silu(gate_part) * up_part).astype(jnp.bfloat16)
            out = jnp.dot(hidden, down_proj[e], preferred_element_type=jnp.float32).astype(jnp.bfloat16)
            outs.append(out.reshape(total // slab, capacity, model_width))
        out = jnp.stack(outs, 1).reshape(total, model_width)
        expert_out = scatter_sum_tp([out[i * rows : (i + 1) * rows] for i in range(lanes)])
        expert_out = expert_out.astype(jnp.bfloat16)
        for i, d in enumerate(members):
            returned[d] = swap(expert_out[i * slab : (i + 1) * slab], "sp", d)
    returned = jnp.concatenate(returned)
    moe = jnp.dot(mixing, returned, preferred_element_type=jnp.float32)
    moe = moe[:own_rows] + moe[own_rows:]
    final = deep_alpha * x_one.astype(jnp.float32) + moe
    return layer_norm_gain(final, norm2_gain).astype(jnp.bfloat16)


def solution(mesh):
    in_specs = (
        P(("sp", "tp"), None),
        P("sp", "tp"),
        P("sp", "tp"),
        P("sp", "tp"),
        P(),
        P(),
        P("tp", None),
        P(),
        P(),
        P(("sp", "tp"), None),
        P(("sp", "tp")),
        P(("sp", "tp"), None),
        P("sp", None, "tp"),
        P("sp", None, "tp"),
        P("sp", "tp", None),
    )
    out_specs = P(("sp", "tp"), None)
    return jax.shard_map(
        per_device, mesh=mesh, in_specs=in_specs, out_specs=out_specs, check_vma=False
    )
```

```python
import functools
import math

import jax
import jax.numpy as jnp
import numpy as np
from jax import lax
from jax.experimental import pallas as pl
from jax.experimental.pallas import tpu as pltpu
from jax.sharding import PartitionSpec as P

GRID_W = 64


deep_alpha = 2.0**0.5
rope_theta = 10000.0


def swap(block, axis, bits):
    if bits == 0:
        return block
    count = lax.axis_size(axis)
    return lax.ppermute(block, axis, [(i, i ^ bits) for i in range(count)])


def rotary_tables(head_size, total):
    half = head_size // 2
    inv_freq = np.float32(rope_theta) ** (-np.arange(0, half, 2, dtype=np.float32) / half)

    def spread(count, first):
        angle = np.arange(count, dtype=np.float32)[:, None] * inv_freq
        cosine = np.zeros((count, head_size), np.float32)
        sine = np.zeros((count, head_size), np.float32)
        for offset, sign in ((0, -1), (half, 1)):
            lanes = slice(offset + first, offset + first + half // 2)
            cosine[:, lanes] = np.cos(angle)
            sine[:, lanes] = sign * np.sin(angle)
        return jnp.asarray(cosine), jnp.asarray(sine)

    row_cosine, row_sine = spread(-(-total // GRID_W), 0)
    col_cosine, col_sine = spread(GRID_W, half // 2)
    return row_cosine, row_sine, col_cosine, col_sine


def table_rows(row_ref, col_ref, start, count):
    span = math.gcd(count, GRID_W)
    parts = []
    for i in range(count // span):
        token = start + i * span
        row = row_ref[pl.ds(token // GRID_W, 1), :]
        parts.append(row + col_ref[pl.ds(token % GRID_W, span), :])
    return jnp.concatenate(parts, 0) if len(parts) > 1 else parts[0]


def normed_turned(block, gain, cosine, sine):
    values32 = block.astype(jnp.float32)
    normed = values32 * lax.rsqrt(jnp.mean(values32 * values32, -1, keepdims=True) + 1e-06) * gain
    half = normed.shape[-1] // 2
    turned = normed * cosine + pltpu.roll(normed, half, 1) * sine
    return turned.astype(jnp.bfloat16)


def key_kernel(kv_local, place_ref, key_ref, value_ref, gain_ref, rc, rs, cc, cs, out_ref):
    tokens, width = key_ref.shape
    head_size = width // kv_local
    start = place_ref[0] * tokens
    cosine = table_rows(rc, cc, start, tokens)
    sine = table_rows(rs, cs, start, tokens)
    for h in range(kv_local):
        lanes = slice(h * head_size, (h + 1) * head_size)
        out_ref[:, lanes] = normed_turned(key_ref[:, lanes], gain_ref[...], cosine, sine)
    out_ref[:, width:] = value_ref[...]


def rotated_keys_values(place, keys, values, gain, tables, kv_local):
    smem = pl.BlockSpec(memory_space=pltpu.SMEM)
    vmem = pl.BlockSpec(memory_space=pltpu.VMEM)
    return pl.pallas_call(
        functools.partial(key_kernel, kv_local),
        in_specs=[smem] + [vmem] * 7,
        out_specs=vmem,
        out_shape=jax.ShapeDtypeStruct((keys.shape[0], 2 * keys.shape[1]), jnp.bfloat16),
        name="rotate_keys",
    )(place, keys, values, gain[None], *tables)


def layer_norm_gain(summed, gain):
    centre = summed - jnp.mean(summed, -1, keepdims=True)
    spread = jnp.mean(centre * centre, -1, keepdims=True)
    return centre * lax.rsqrt(spread + 1e-06) * gain


def attention_kernel(scale, chunks, lanes, place_ref, query_ref, gain_ref, rc, rs, cc, cs, *refs):
    key_refs = refs[:chunks]
    value_refs = refs[chunks : 2 * chunks]
    out_ref = refs[2 * chunks]
    tokens = query_ref.shape[0]
    rows = tokens // lanes
    query = []
    for lane in range(lanes):
        first = (place_ref[1] ^ lane) * rows
        start = place_ref[0] * tokens + first
        query.append(
            normed_turned(
                query_ref[pl.ds(pl.multiple_of(first, rows), rows), :],
                gain_ref[...],
                table_rows(rc, cc, start, rows),
                table_rows(rs, cs, start, rows),
            )
        )
    query = jnp.concatenate(query, 0)
    scores = [
        lax.dot_general(
            query, key[...], (((1,), (1,)), ((), ())), preferred_element_type=jnp.float32
        )
        for key in key_refs
    ]
    row_max = functools.reduce(jnp.maximum, [jnp.max(s, -1, keepdims=True) for s in scores])
    row_sum = jnp.zeros_like(row_max)
    weighted = jnp.zeros(out_ref.shape, jnp.float32)
    for block, value in zip(scores, value_refs):
        probs = jnp.exp2((block - row_max) * (scale * math.log2(math.e)))
        row_sum = row_sum + jnp.sum(probs, -1, keepdims=True)
        weighted = weighted + jnp.dot(
            probs.astype(jnp.bfloat16), value[...], preferred_element_type=jnp.float32
        )
    out_ref[...] = (weighted / row_sum).astype(out_ref.dtype)


def attention(place, query, gain, tables, pieces, kv_local, lanes):
    rows, width = query.shape
    head_size = gain.shape[0]
    heads = width // head_size
    group = heads // kv_local
    count = len(pieces)
    tokens = pieces[0].shape[0]

    def whole(array):
        return pl.BlockSpec(array.shape, lambda h: (0, 0))

    query_spec = pl.BlockSpec((rows, head_size), lambda h: (0, h))
    key_spec = pl.BlockSpec((tokens, head_size), lambda h: (0, h // group))
    value_spec = pl.BlockSpec((tokens, head_size), lambda h: (0, kv_local + h // group))
    gain = gain[None]
    return pl.pallas_call(
        functools.partial(attention_kernel, head_size ** (-0.5), count, lanes),
        grid=(heads,),
        in_specs=[pl.BlockSpec(memory_space=pltpu.SMEM), query_spec, whole(gain)]
        + [whole(t) for t in tables]
        + [key_spec] * count
        + [value_spec] * count,
        out_specs=query_spec,
        out_shape=jax.ShapeDtypeStruct((rows, width), jnp.bfloat16),
        compiler_params=pltpu.CompilerParams(vmem_limit_bytes=56 * 1024 * 1024),
        cost_estimate=pl.CostEstimate(
            flops=4 * rows * count * tokens * width, transcendentals=0, bytes_accessed=0
        ),
        name="attention",
    )(place, query, gain, *tables, *pieces, *pieces)


def expert_kernel(half, lanes, *refs):
    token_refs = refs[:lanes]
    gate_ref, up_ref, down_ref = refs[lanes : lanes + 3]
    out_refs = refs[lanes + 3 : 2 * lanes + 3]
    gate_sum, up_sum, hidden_ref = refs[2 * lanes + 3 :]
    step = pl.program_id(0)
    rows = token_refs[0].shape[0]

    @pl.when(step < half)
    def _():
        tokens = jnp.concatenate([r[...] for r in token_refs], 0)
        gate_part = jnp.dot(tokens, gate_ref[...], preferred_element_type=jnp.float32)
        up_part = jnp.dot(tokens, up_ref[...], preferred_element_type=jnp.float32)

        @pl.when(step == 0)
        def _():
            gate_sum[...] = gate_part
            up_sum[...] = up_part

        @pl.when(step > 0)
        def _():
            gate_sum[...] += gate_part
            up_sum[...] += up_part

    @pl.when(step == half - 1)
    def _():
        gate = gate_sum[...]
        hidden_ref[...] = (gate / (1.0 + jnp.exp(-gate)) * up_sum[...]).astype(jnp.bfloat16)

    @pl.when(step >= half)
    def _():
        out = jnp.dot(hidden_ref[...], down_ref[...], preferred_element_type=jnp.float32)
        out = out.astype(jnp.bfloat16)
        for i, ref in enumerate(out_refs):
            ref[...] = out[i * rows : (i + 1) * rows]


def expert(tokens, gate, up, down):
    lanes = len(tokens)
    rows, width = tokens[0].shape
    hidden = gate.shape[1]
    half = 4
    block = width // half
    token_spec = pl.BlockSpec((rows, block), lambda i: (0, jnp.minimum(i, half - 1)))
    weight_spec = pl.BlockSpec((block, hidden), lambda i: (jnp.minimum(i, half - 1), 0))
    down_spec = pl.BlockSpec((hidden, block), lambda i: (0, jnp.maximum(i - half, 0)))
    out_spec = pl.BlockSpec((rows, block), lambda i: (0, jnp.maximum(i - half, 0)))
    total = rows * lanes
    return pl.pallas_call(
        functools.partial(expert_kernel, half, lanes),
        grid=(2 * half,),
        in_specs=[token_spec] * lanes + [weight_spec, weight_spec, down_spec],
        out_specs=[out_spec] * lanes,
        out_shape=[jax.ShapeDtypeStruct((rows, width), jnp.bfloat16)] * lanes,
        scratch_shapes=[
            pltpu.VMEM((total, hidden), jnp.float32),
            pltpu.VMEM((total, hidden), jnp.float32),
            pltpu.VMEM((total, hidden), jnp.bfloat16),
        ],
        compiler_params=pltpu.CompilerParams(vmem_limit_bytes=24 * 1024 * 1024),
        cost_estimate=pl.CostEstimate(
            flops=6 * total * width * hidden, transcendentals=0, bytes_accessed=0
        ),
        name="expert",
    )(*tokens, gate, up, down)


def gather_swapped(block, axis):
    count = lax.axis_size(axis)
    got = {0: block}
    for bits in range(0, count, 2):
        got[bits] = swap(block, axis, bits)
        got[bits ^ 1] = swap(got[bits], axis, 1)
    return [got[i] for i in range(count)]


def gather_tp(block):
    have = [block]
    step = lax.axis_size("tp") // 2
    found = {0: block}
    while step:
        for key in list(found):
            found[key ^ step] = swap(found[key], "tp", step)
        step //= 2
    return [found[i] for i in range(lax.axis_size("tp"))]


def scatter_sum_tp(parts):
    step = 1
    parts = dict(enumerate(parts))
    while len(parts) > 1:
        sent = {k: swap(v.astype(jnp.bfloat16), "tp", step) for k, v in parts.items() if k & step}
        parts = {
            k: v.astype(jnp.bfloat16).astype(jnp.float32) + sent[k | step].astype(jnp.float32)
            for k, v in parts.items()
            if not k & step
        }
        step *= 2
    return parts[0]


def per_device(
    resid,
    queries,
    keys,
    values,
    q_gain,
    key_norm_gain,
    out_weight,
    norm1_gain,
    norm2_gain,
    expert_ids,
    group_weight,
    expert_weight,
    gate_proj,
    up_proj,
    down_proj,
):
    local_tokens = queries.shape[0]
    head_size = q_gain.shape[0]
    kv_local = keys.shape[1] // head_size
    model_width = resid.shape[1]
    sp_count = lax.axis_size("sp")
    lanes = lax.axis_size("tp")
    own_rows = local_tokens // lanes
    own_sp = lax.axis_index("sp")
    own_tp = lax.axis_index("tp")

    place = jnp.stack([own_sp, own_tp]).astype(jnp.int32)
    tables = rotary_tables(head_size, local_tokens * sp_count)
    pieces = gather_swapped(
        rotated_keys_values(place, keys, values, key_norm_gain, tables, kv_local), "sp"
    )
    per = max(1, sp_count // 8)
    if per > 1:
        pieces = [jnp.concatenate(pieces[i : i + per]) for i in range(0, sp_count, per)]

    top_count = expert_ids.shape[1]
    expert_local = gate_proj.shape[0]
    expert_total = expert_local * sp_count
    capacity = (3 * top_count * own_rows + 2 * expert_total - 1) // (2 * expert_total)
    flat_ids = expert_ids.reshape(-1)
    one_hot = (flat_ids[:, None] == jnp.arange(expert_total, dtype=jnp.int32)[None, :]).astype(
        jnp.float32
    )
    places = jnp.arange(flat_ids.shape[0], dtype=jnp.int32)
    before = (places[None, :] < places[:, None]).astype(jnp.float32)
    rank = jnp.sum(jnp.dot(before, one_hot) * one_hot, 1).astype(jnp.int32)
    swapped_ids = (flat_ids // expert_local ^ own_sp) * expert_local + flat_ids % expert_local
    slot = (swapped_ids * capacity + rank).reshape(own_rows, top_count)
    slots = expert_total * capacity
    hit = slot[..., None] == jnp.arange(slots, dtype=jnp.int32)
    placing = jnp.sum(hit.astype(jnp.float32), 1).astype(jnp.bfloat16)
    gates = group_weight[:, None] * expert_weight / jnp.sum(expert_weight, -1, keepdims=True)
    mixing = jnp.sum(jnp.where(hit, gates[..., None], 0.0), 1)
    mixing_high = mixing.astype(jnp.bfloat16)
    mixing_low = (mixing - mixing_high.astype(jnp.float32)).astype(jnp.bfloat16)
    mixing = jnp.concatenate([mixing_high, mixing_low])

    attn = attention(place, queries, q_gain, tables, pieces, kv_local, lanes)
    partial = [
        jnp.dot(
            attn[i * own_rows : (i + 1) * own_rows], out_weight, preferred_element_type=jnp.float32
        )
        for i in range(lanes)
    ]
    proj = scatter_sum_tp(partial).astype(jnp.bfloat16)
    summed = deep_alpha * resid.astype(jnp.float32) + proj.astype(jnp.float32)
    x_one = layer_norm_gain(summed, norm1_gain).astype(jnp.bfloat16)

    outgoing = lax.dot_general(
        placing, x_one, (((0,), (0,)), ((), ())), preferred_element_type=jnp.float32
    ).astype(jnp.bfloat16)
    slab = expert_local * capacity
    groups = min(4, sp_count)
    per_group = sp_count // groups
    arrived = [swap(outgoing[d * slab : (d + 1) * slab], "sp", d) for d in range(sp_count)]
    returned = [None] * sp_count
    for g in range(groups):
        members = range(g * per_group, (g + 1) * per_group)
        block = jnp.concatenate([arrived[d] for d in members])
        rows = block.shape[0]
        pieces = gather_tp(block)
        by_expert = [
            p.reshape(rows // slab, expert_local, capacity, model_width) for p in pieces
        ]
        outs = []
        for e in range(expert_local):
            tokens = [b[:, e].reshape(rows // expert_local, model_width) for b in by_expert]
            outs.append(expert(tokens, gate_proj[e], up_proj[e], down_proj[e]))
        if expert_local > 1:
            outs = [
                jnp.stack([o.reshape(rows // slab, capacity, model_width) for o in part], 1)
                for part in zip(*outs)
            ]
        else:
            outs = outs[0]
        expert_out = scatter_sum_tp([o.reshape(rows, model_width) for o in outs])
        expert_out = expert_out.astype(jnp.bfloat16)
        for i, d in enumerate(members):
            returned[d] = swap(expert_out[i * slab : (i + 1) * slab], "sp", d)
    returned = jnp.concatenate(returned)
    moe = jnp.dot(mixing, returned, preferred_element_type=jnp.float32)
    moe = moe[:own_rows] + moe[own_rows:]
    final = deep_alpha * x_one.astype(jnp.float32) + moe
    return layer_norm_gain(final, norm2_gain).astype(jnp.bfloat16)


def solution(mesh):
    in_specs = (
        P(("sp", "tp"), None),
        P("sp", "tp"),
        P("sp", "tp"),
        P("sp", "tp"),
        P(),
        P(),
        P("tp", None),
        P(),
        P(),
        P(("sp", "tp"), None),
        P(("sp", "tp")),
        P(("sp", "tp"), None),
        P("sp", None, "tp"),
        P("sp", None, "tp"),
        P("sp", "tp", None),
    )
    out_specs = P(("sp", "tp"), None)
    return jax.shard_map(
        per_device, mesh=mesh, in_specs=in_specs, out_specs=out_specs, check_vma=False
    )
```
